32 devices in a mesh: fs: 4 (over z), rep: 2 (over y), tp: 4 (over x, core).
Axes of the slice: x: 2, y: 2, z: 4, core: 2. Of those that a mesh axis runs over, the one named last changes fastest.
Arguments:
- saved_input: bfloat16 [5120, 3072], P(('fs', 'rep')), may hold values from -6 to 6
- key_cotangent: bfloat16 [5120, 1024], P(('fs', 'rep'), 'tp'), may hold values from -0.0625 to 0.0625
- value_cotangent: bfloat16 [5120, 2048], P(('fs', 'rep'), 'tp'), may hold values from -0.0625 to 0.0625
- key_factor: bfloat16 [3072, 256], replicated, may hold values from -0.375 to 0.375
- value_factor: bfloat16 [3072, 256], replicated, may hold values from -0.375 to 0.375
- key_weight: float32 [3072, 1024], P(('fs', 'rep'), 'tp'), may hold values from -0.109375 to 0.109375
- value_weight: float32 [3072, 2048], P(('fs', 'rep'), 'tp'), may hold values from -0.109375 to 0.109375
- key_first: float32 [256, 1024], P(None, 'tp'), as said below
- key_second: float32 [256, 1024], P(None, 'tp'), may hold values from 0.05 to 1
- value_first: float32 [256, 2048], P(None, 'tp'), as said below
- value_second: float32 [256, 2048], P(None, 'tp'), may hold values from 0.05 to 1
Outputs:
- key_weight_new: float32 [3072, 1024], P(('fs', 'rep'), 'tp')
- value_weight_new: float32 [3072, 2048], P(('fs', 'rep'), 'tp')
- key_first_new: float32 [256, 1024], P(None, 'tp')
- key_second_new: float32 [256, 1024], P(None, 'tp')
- value_first_new: float32 [256, 2048], P(None, 'tp')
- value_second_new: float32 [256, 2048], P(None, 'tp')
- key_step: float32 [3072, 1024], P(('fs', 'rep'), 'tp')
- value_step: float32 [3072, 2048], P(('fs', 'rep'), 'tp')
- key_copy: bfloat16 [3072, 1024], P(None, 'tp')
- value_copy: bfloat16 [3072, 2048], P(None, 'tp')
The draws below stay inside these ranges and needn't reach their ends.
Inputs may be any that keep to these rules, and one draw needn't show every extreme that they name: `key_first`: real-valued moments whose scale differs from head to head. `value_first`: real-valued moments whose scale differs from head to head.
All inputs are finite; a program needn't handle non-finite values.
Results may differ from the reference program's by a relative error of at most 0.004.
Values may be sent and summed in bfloat16 or wider, within the bound.
A program may use at most 64 MiB of HBM per device.

```python
import math
import jax
import jax.numpy as jnp
from jax import lax

D = 3072
HEADS = 8
HK = 128
HV = 256
DK = 1024
DV = 2048
RK = 256
RV = 256
TOKENS = 5120


def head_scaled(key, row_count, head_count, head_width):
    scale_key, value_key = jax.random.split(key)
    spread = jnp.exp(jax.random.uniform(scale_key, (head_count,), jnp.float32, -1.4, 1.4))
    entries = jax.random.normal(value_key, (row_count, head_count, head_width), jnp.float32)
    return (entries * spread[None, :, None]).reshape(row_count, head_count * head_width)


def draw_key_first(key, part):
    return head_scaled(jax.random.fold_in(key, 3), RK, HEADS, HK)


def draw_value_first(key, part):
    return head_scaled(jax.random.fold_in(key, 7), RV, HEADS, HV)


def spiked(values, key, source, target, shards_of, factor):
    owner, partner = [(jnp.arange(values.shape[position]) // (values.shape[position] // shards_of)).reshape([-1 if axis == position else 1 for axis in range(values.ndim)]) for position in (source, target)]
    chosen = jax.random.permutation(key, shards_of)[partner]
    strong = (owner == chosen) | (owner == (partner + shards_of // 2) % shards_of)
    return jnp.where(strong, factor * values, values)


def steps_of(stream_key, extent, shards, smallest, largest):
    factor_of, own = 1.0, jax.random.fold_in(stream_key, 6)
    for axis_at, blocks in shards:
        draws = jnp.exp(jax.random.uniform(jax.random.fold_in(own, axis_at), (blocks,), jnp.float32, smallest / len(shards), largest / len(shards)))
        factor_of = factor_of * jnp.repeat(draws, extent[axis_at] // blocks).reshape([-1 if axis == axis_at else 1 for axis in range(len(extent))])
    return factor_of


def centred(rng, dims, deviation, limit, cuts=(), dtype=jnp.bfloat16):
    loudness = steps_of(rng, dims, cuts, -0.22, 0.18) if cuts else 1.0
    values = jax.random.normal(rng, dims, jnp.float32) * deviation * loudness
    return jnp.minimum(jnp.maximum(values, -limit), limit).astype(dtype)


def heavy_noise(own_key, shape, width, most, cuts, heavy, held_as=jnp.bfloat16):
    values = width * jax.random.normal(own_key, shape, jnp.float32)
    if cuts:
        values = values * steps_of(own_key, shape, cuts, -0.22, 0.18)
    return jnp.clip(spiked(values, jax.random.fold_in(own_key, 3), *heavy), -most, most).astype(held_as)


def setup_inputs(seed: int = 0) -> dict:
    streams_of = jax.random.split(jax.random.key(seed), 12)
    saved_input = heavy_noise(streams_of[0], (TOKENS, D), 1.0, 6.0, ((0, 8),), (0, 1, 8, 2.0))
    key_cotangent = centred(streams_of[1], (TOKENS, DK), ((D * TOKENS // RK) ** -0.5), 0.0625, ((0, 8), (1, 4)))
    value_cotangent = centred(streams_of[2], (TOKENS, DV), ((D * TOKENS // RV) ** -0.5), 0.0625, ((0, 8), (1, 4)))
    key_factor = centred(streams_of[3], (D, RK), RK ** -0.5, 0.375)
    value_factor = centred(streams_of[4], (D, RV), RV ** -0.5, 0.375)
    key_weight = centred(streams_of[5], (D, DK), D ** -0.5, 0.109375, ((0, 8), (1, 4)), jnp.float32)
    value_weight = centred(streams_of[6], (D, DV), D ** -0.5, 0.109375, ((0, 8), (1, 4)), jnp.float32)
    key_first = draw_key_first(jax.random.fold_in(streams_of[11], 71), 0)
    key_second = jnp.clip(jnp.exp(math.log(1.0) - 2.9957323 * jax.random.uniform(streams_of[8], (RK, DK), jnp.float32) ** steps_of(streams_of[8], (RK, DK), ((1, 4),), -0.2, 0.2)), 0.05, 1.0)
    value_first = draw_value_first(jax.random.fold_in(streams_of[11], 71), 0)
    value_second = jnp.clip(jnp.exp(math.log(1.0) - 2.9957323 * jax.random.uniform(streams_of[10], (RV, DV), jnp.float32) ** steps_of(streams_of[10], (RV, DV), ((1, 4),), -0.2, 0.2)), 0.05, 1.0)
    return dict(saved_input=saved_input, key_cotangent=key_cotangent, value_cotangent=value_cotangent, key_factor=key_factor, value_factor=value_factor, key_weight=key_weight, value_weight=value_weight, key_first=key_first, key_second=key_second, value_first=value_first, value_second=value_second)


first_decay = 0.8
second_decay = 0.9
epsilon = 1e-08
learn_rate = 0.01

def projected(saved_input, cotangent, factor):
    basis = jnp.dot(saved_input, factor, preferred_element_type=jnp.float32)
    return lax.dot_general(basis, cotangent.astype(jnp.float32), (((0,), (0,)), ((), ())), precision=lax.Precision.HIGHEST)

def moments(projection, first, second):
    first_new = first_decay * first + (1.0 - first_decay) * projection
    second_new = second_decay * second + (1.0 - second_decay) * projection * projection
    normed = first_new / (jnp.sqrt(second_new) + epsilon)
    return (first_new, second_new, normed)

def reference(saved_input, key_cotangent, value_cotangent, key_factor, value_factor, key_weight, value_weight, key_first, key_second, value_first, value_second):
    key_projected = projected(saved_input, key_cotangent, key_factor)
    value_projected = projected(saved_input, value_cotangent, value_factor)
    key_first_new, key_second_new, key_normed = moments(key_projected, key_first, key_second)
    value_first_new, value_second_new, value_normed = moments(value_projected, value_first, value_second)
    squares = jnp.sum(key_normed * key_normed) + jnp.sum(value_normed * value_normed)
    entries = jnp.float32(RK * DK + RV * DV)
    shrink = jnp.sqrt(entries / (entries + squares))
    key_step = shrink * jnp.dot(key_factor.astype(jnp.float32), key_normed, precision=lax.Precision.HIGHEST)
    value_step = shrink * jnp.dot(value_factor.astype(jnp.float32), value_normed, precision=lax.Precision.HIGHEST)
    key_weight_new = key_weight - learn_rate * key_step
    value_weight_new = value_weight - learn_rate * value_step
    return (key_weight_new, value_weight_new, key_first_new, key_second_new, value_first_new, value_second_new, key_step, value_step, key_weight_new.astype(jnp.bfloat16), value_weight_new.astype(jnp.bfloat16))
```

```python
import functools
import math

import jax
import jax.numpy as jnp
from jax import lax
from jax.experimental import pallas as pl
from jax.experimental.pallas import tpu as pltpu
from jax.sharding import PartitionSpec as P

first_decay = 0.8
second_decay = 0.9
epsilon = 1e-08
learn_rate = 0.01

SCATTER_TYPE = jnp.float32
GATHER_TYPE = jnp.float32
MESH = pl.DeviceIdType.MESH


def moments(projection, first, second):
    first_new = first_decay * first + (1.0 - first_decay) * projection
    second_new = second_decay * second + (1.0 - second_decay) * projection * projection
    normed = first_new / (jnp.sqrt(second_new) + epsilon)
    return (first_new, second_new, normed)


def contract(basis, cotangent):
    upper = basis.astype(jnp.bfloat16)
    lower = (basis - upper.astype(jnp.float32)).astype(jnp.bfloat16)
    dims = (((0,), (0,)), ((), ()))
    high_part = lax.dot_general(upper, cotangent, dims, preferred_element_type=jnp.float32)
    low_part = lax.dot_general(lower, cotangent, dims, preferred_element_type=jnp.float32)
    return high_part + low_part


class Plan:
    def __init__(self, mesh_shape, rows, rank, key_cols, value_cols):
        self.F, self.R, self.T = (mesh_shape[a] for a in ("fs", "rep", "tp"))
        self.rows, self.rank = rows, rank
        self.kc, self.vc = key_cols, value_cols
        self.cols = key_cols + value_cols
        self.piece = math.gcd(rows, 64)
        self.pieces = rows // self.piece
        self.dup = 1 if self.R == 2 and self.pieces >= 4 else 0
        self.half = self.rank // self.R
        owners = self.F
        while self.half % owners or (self.half // owners) % 16 or self.F % owners:
            owners -= 1
        self.owners = owners
        self.slice = self.half // owners


def kernel(
    plan,
    x_hbm, kcot_hbm, vcot_hbm, kfac_hbm, vfac_hbm, kw, vw, kf, ks, vf, vs,
    wall, kf_out, ks_out, vf_out, vs_out, normed_out, squares_out,
    x, kcot, vcot, kfac, vfac, partial, ysend, yrecv, half, zsend, zrecv, total, sq,
    load_sem, zs_sem, zr_sem, ys_sem, yr_sem, ds_sem, dr_sem,
    rys, ryr, rzs, rzr, gzs, gzr, gys, gyr, ts, tr,
):
    F, R, T = plan.F, plan.R, plan.T
    NP, PR, C = plan.pieces, plan.piece, plan.cols
    z = lax.axis_index("fs")
    y = lax.axis_index("rep")
    t = lax.axis_index("tp")

    loads = [
        pltpu.make_async_copy(s, d, load_sem.at[i])
        for i, (s, d) in enumerate(
            ((x_hbm, x), (kfac_hbm, kfac), (kcot_hbm, kcot), (vfac_hbm, vfac), (vcot_hbm, vcot))
        )
    ]
    for c in loads:
        c.start()

    def fs_peer(j):
        return lax.rem(z + j, F)

    def rep_peer(j):
        return lax.rem(y + j, R)

    def tp_peer(j):
        return lax.rem(t + j, T)

    barrier = pltpu.get_barrier_semaphore()
    for axis, size, peer in (("fs", F, fs_peer), ("rep", R, rep_peer), ("tp", T, tp_peer)):
        for j in range(1, size):
            pl.semaphore_signal(barrier, 1, device_id={axis: peer(j)}, device_id_type=MESH)

    own = wall.at[z, y]
    own[:, : plan.kc] = kw[...].astype(jnp.bfloat16)
    own[:, plan.kc :] = vw[...].astype(jnp.bfloat16)
    pl.semaphore_wait(barrier, F + R + T - 3)

    def rc(src, dst, s, r, axis, target):
        return pltpu.make_async_remote_copy(
            src_ref=src, dst_ref=dst, send_sem=s, recv_sem=r,
            device_id={axis: target}, device_id_type=MESH,
        )

    def prows(p):
        return pl.ds(p * PR, PR)

    def fs_copy(direction, s, p, wait=False):
        if direction == 0:
            source, target, ok = z - s, z + 1, z < F - 1
        else:
            source, target, ok = z + s, z - 1, z > 0
        source = jnp.clip(source, 0, F - 1)
        target = jnp.clip(target, 0, F - 1)
        ref = wall.at[source, y, prows(p)]
        sem = s if wait else s + 1
        return rc(ref, ref, zs_sem.at[direction, s, p], zr_sem.at[direction, sem, p], "fs", target)

    def dup_copy(direction, s, wait=False):
        if direction == 0:
            source, target = z - s, z + 1
        else:
            source, target = z + s, z - 1
        source = jnp.clip(source, 0, F - 1)
        target = jnp.clip(target, 0, F - 1)
        ref = wall.at[source, 1 - y, prows(0)]
        sem = s if wait else s + 1
        return rc(ref, ref, ds_sem.at[direction, s], dr_sem.at[direction, sem], "fs", target)

    def onward(direction):
        return z < F - 1 if direction == 0 else z > 0

    def arrives(direction, s):
        return z - s >= 0 if direction == 0 else z + s < F

    def rep_copy(source, p, j):
        ref = wall.at[source, y, prows(p)]
        return rc(ref, ref, ys_sem.at[source, p, j], yr_sem.at[source, p, j], "rep", rep_peer(j))

    def rep_arrival(source, p, j):
        ref = wall.at[source, lax.rem(y + R - j, R), prows(p)]
        return rc(ref, ref, ys_sem.at[source, p, j], yr_sem.at[source, p, j], "rep", rep_peer(j))

    def send_own(lo, hi):
        for p in range(lo, hi):
            for j in range(1, R):
                rep_copy(z, p, j).start()
            for d in (0, 1):

                @pl.when(onward(d))
                def _():
                    fs_copy(d, 0, p).start()

    def relay(s, lo, hi):
        if s >= F:
            return
        for p in range(lo, hi):
            for d in (0, 1):

                @pl.when(arrives(d, s))
                def _():
                    source = z - s if d == 0 else z + s
                    fs_copy(d, s, p, wait=True).wait_recv()
                    if s < F - 1:

                        @pl.when(onward(d))
                        def _():
                            fs_copy(d, s, p).start()

                    if not (plan.dup and p == 0):
                        for j in range(1, R):
                            rep_copy(source, p, j).start()

        if plan.dup and hi == NP:
            for d in (0, 1):

                @pl.when(arrives(d, s))
                def _():
                    dup_copy(d, s, wait=True).wait_recv()
                    if s < F - 1:

                        @pl.when(onward(d))
                        def _():
                            dup_copy(d, s).start()

    NH = (NP + 1) // 2
    send_own(0, NH)

    for i in (0, 1, 2):
        loads[i].wait()
    basis = jnp.dot(x[...], kfac[...], preferred_element_type=jnp.float32)
    partial[:, : plan.kc] = contract(basis, kcot[...])
    for i in (3, 4):
        loads[i].wait()
    basis = jnp.dot(x[...], vfac[...], preferred_element_type=jnp.float32)
    partial[:, plan.kc :] = contract(basis, vcot[...])

    H = plan.half
    ysend[...] = partial[...].astype(SCATTER_TYPE)
    for j in range(1, R):
        to = rep_peer(j)
        rc(ysend.at[pl.ds(to * H, H)], yrecv.at[j], rys.at[j], ryr.at[j], "rep", to).start()
    send_own(NH, NP)
    if plan.dup:
        rep_arrival(z, 0, 1).wait_recv()
        for d in (0, 1):

            @pl.when(onward(d))
            def _():
                dup_copy(d, 0).start()

    acc = partial[pl.ds(y * H, H), :]
    for j in range(1, R):
        rc(ysend.at[pl.ds(0, H)], yrecv.at[j], rys.at[j], ryr.at[j], "rep", rep_peer(j)).wait_recv()
        acc = acc + yrecv[j].astype(jnp.float32)
    half[...] = acc
    zsend[...] = acc.astype(SCATTER_TYPE)

    S, O = plan.slice, plan.owners

    def slice_copy(j):
        to = fs_peer(j)
        rows = pl.ds(jnp.minimum(to, O - 1) * S, S)
        return rc(zsend.at[rows], zrecv.at[j], rzs.at[j], rzr.at[j], "fs", to)

    for j in range(1, F):

        @pl.when(fs_peer(j) < O)
        def _():
            slice_copy(j).start()

    relay(1, 0, NH)

    mine = pl.ds(y * H + jnp.minimum(z, O - 1) * S, S)

    def sum_copy(j):
        return rc(total.at[mine], total.at[mine], gzs.at[j], gzr.at[j], "fs", fs_peer(j))

    @pl.when(z < O)
    def _():
        acc = half[pl.ds(jnp.minimum(z, O - 1) * S, S), :]
        for j in range(1, F):
            slice_copy(j).wait_recv()
            acc = acc + zrecv[j].astype(jnp.float32)
        total[mine, :] = acc.astype(GATHER_TYPE)
        for j in range(1, F):
            sum_copy(j).start()

    relay(1, NH, NP)

    for j in range(1, F):
        src = lax.rem(z + F - j, F)

        @pl.when(src < O)
        def _():
            rows = pl.ds(y * H + jnp.minimum(src, O - 1) * S, S)
            rc(total.at[rows], total.at[rows], gzs.at[j], gzr.at[j], "fs", fs_peer(j)).wait_recv()

    def half_copy(j):
        rows = pl.ds(y * H, H)
        return rc(total.at[rows], total.at[rows], gys.at[j], gyr.at[j], "rep", rep_peer(j))

    for j in range(1, R):
        half_copy(j).start()

    relay(2, 0, NH)

    for j in range(1, R):
        rows = pl.ds(lax.rem(y + R - j, R) * H, H)
        rc(total.at[rows], total.at[rows], gys.at[j], gyr.at[j], "rep", rep_peer(j)).wait_recv()

    proj = total[:, : plan.kc].astype(jnp.float32)
    first_new, second_new, normed = moments(proj, kf[...], ks[...])
    kf_out[...] = first_new
    ks_out[...] = second_new
    normed_out[:, : plan.kc] = normed
    squares = jnp.sum(normed * normed, axis=0, keepdims=True)
    squares = jnp.sum(squares, axis=1, keepdims=True)
    proj = total[:, plan.kc :].astype(jnp.float32)
    first_new, second_new, normed = moments(proj, vf[...], vs[...])
    vf_out[...] = first_new
    vs_out[...] = second_new
    normed_out[:, plan.kc :] = normed
    more = jnp.sum(normed * normed, axis=0, keepdims=True)
    squares = squares + jnp.sum(more, axis=1, keepdims=True)
    sq[t] = jnp.broadcast_to(squares, (8, 128))

    def sq_copy(j):
        return rc(sq.at[t], sq.at[t], ts.at[j], tr.at[j], "tp", tp_peer(j))

    for j in range(1, T):
        sq_copy(j).start()

    relay(2, NH, NP)

    for j in range(1, T):
        src = lax.rem(t + T - j, T)
        rc(sq.at[src], sq.at[src], ts.at[j], tr.at[j], "tp", tp_peer(j)).wait_recv()
    acc = sq[0]
    for i in range(1, T):
        acc = acc + sq[i]
    squares_out[...] = acc

    for s in range(3, F):
        relay(s, 0, NP)

    for source in range(F):
        for p in range(NP):
            for j in range(1, R):
                if plan.dup and p == 0:

                    @pl.when(z == source)
                    def _():
                        rep_copy(source, p, j).wait_send()
                else:
                    rep_arrival(source, p, j).wait_recv()
                    rep_copy(source, p, j).wait_send()
    for s in range(F - 1):
        for d in (0, 1):

            @pl.when(jnp.logical_and(arrives(d, s), onward(d)))
            def _():
                for p in range(NP):
                    fs_copy(d, s, p).wait_send()
                if plan.dup:
                    dup_copy(d, s).wait_send()
    for j in range(1, R):
        rc(ysend.at[pl.ds(0, H)], yrecv.at[j], rys.at[j], ryr.at[j], "rep", rep_peer(j)).wait_send()
        half_copy(j).wait_send()
    for j in range(1, F):

        @pl.when(fs_peer(j) < O)
        def _():
            slice_copy(j).wait_send()

        @pl.when(z < O)
        def _():
            sum_copy(j).wait_send()
    for j in range(1, T):
        sq_copy(j).wait_send()


def exchange(plan, *args):
    x, kcot, vcot, kfac, vfac = args[:5]
    F, R, T, NP, C = plan.F, plan.R, plan.T, plan.pieces, plan.cols
    f32 = jnp.float32
    vmem = pl.BlockSpec(memory_space=pltpu.VMEM)
    hbm = pl.BlockSpec(memory_space=pl.ANY)
    dma = pltpu.SemaphoreType.DMA
    rank = plan.rank
    out_shape = (
        jax.ShapeDtypeStruct((F, R, plan.rows, C), jnp.bfloat16),
        jax.ShapeDtypeStruct((rank, plan.kc), f32),
        jax.ShapeDtypeStruct((rank, plan.kc), f32),
        jax.ShapeDtypeStruct((rank, plan.vc), f32),
        jax.ShapeDtypeStruct((rank, plan.vc), f32),
        jax.ShapeDtypeStruct((rank, C), f32),
        jax.ShapeDtypeStruct((8, 128), f32),
    )
    scratch = [pltpu.VMEM(a.shape, a.dtype) for a in (x, kcot, vcot, kfac, vfac)]
    scratch += [
        pltpu.VMEM((rank, C), f32),
        pltpu.VMEM((rank, C), SCATTER_TYPE),
        pltpu.VMEM((R, plan.half, C), SCATTER_TYPE),
        pltpu.VMEM((plan.half, C), f32),
        pltpu.VMEM((plan.half, C), SCATTER_TYPE),
        pltpu.VMEM((F, plan.slice, C), SCATTER_TYPE),
        pltpu.VMEM((rank, C), GATHER_TYPE),
        pltpu.VMEM((T, 8, 128), f32),
        dma((5,)),
        dma((2, F, NP)),
        dma((2, F, NP)),
        dma((F, NP, R)),
        dma((F, NP, R)),
        dma((2, F)),
        dma((2, F)),
        dma((R,)), dma((R,)),
        dma((F,)), dma((F,)),
        dma((F,)), dma((F,)),
        dma((R,)), dma((R,)),
        dma((T,)), dma((T,)),
    ]
    return pl.pallas_call(
        functools.partial(kernel, plan),
        out_shape=out_shape,
        in_specs=[hbm] * 5 + [vmem] * 6,
        out_specs=[vmem] * 7,
        scratch_shapes=scratch,
        compiler_params=pltpu.CompilerParams(
            collective_id=0, has_side_effects=True, vmem_limit_bytes=48 * 1024 * 1024
        ),
    )(*args)


def body(mesh_shape, *args):
    (x, kcot, vcot, kfac, vfac, kw, vw, kf, ks, vf, vs) = args
    rows, key_cols = kw.shape
    value_cols = vw.shape[1]
    plan = Plan(mesh_shape, rows, kf.shape[0], key_cols, value_cols)
    wall, kf_new, ks_new, vf_new, vs_new, normed, squares = exchange(plan, *args)
    T = plan.T
    entries = jnp.float32(kf.size * T + vf.size * T)
    shrink = jnp.sqrt(entries / (entries + squares[0, 0]))

    row_offset = lax.axis_index(("fs", "rep")) * rows
    upper = normed.astype(jnp.bfloat16)
    lower = (normed - upper.astype(jnp.float32)).astype(jnp.bfloat16)

    def one(factor, weight, lo, hi):
        mine = lax.dynamic_slice_in_dim(factor, row_offset, rows, 0)
        step = jnp.dot(mine, upper[:, lo:hi], preferred_element_type=jnp.float32)
        step = step + jnp.dot(mine, lower[:, lo:hi], preferred_element_type=jnp.float32)
        step = shrink * step
        weight_new = weight - learn_rate * step
        everywhere = wall.reshape(-1, plan.cols)[:, lo:hi].astype(jnp.float32)
        full = jnp.dot(factor, upper[:, lo:hi], preferred_element_type=jnp.float32)
        copy = (everywhere - learn_rate * (shrink * full)).astype(jnp.bfloat16)
        return weight_new, step, copy

    k_new, k_step, k_copy = one(kfac, kw, 0, plan.kc)
    v_new, v_step, v_copy = one(vfac, vw, plan.kc, plan.cols)
    return (k_new, v_new, kf_new, ks_new, vf_new, vs_new, k_step, v_step, k_copy, v_copy)


def solution(mesh):
    rows = P(("fs", "rep"), "tp")
    cols = P(None, "tp")
    in_specs = (P(("fs", "rep"), None), rows, rows, P(), P(), rows, rows, cols, cols, cols, cols)
    out_specs = (rows, rows, cols, cols, cols, cols, rows, rows, cols, cols)
    return jax.shard_map(
        functools.partial(body, dict(mesh.shape)),
        mesh=mesh, in_specs=in_specs, out_specs=out_specs, check_vma=False,
    )
```

```python
import functools
import math

import jax
import jax.numpy as jnp
from jax import lax
from jax.experimental import pallas as pl
from jax.experimental.pallas import tpu as pltpu
from jax.sharding import PartitionSpec as P

first_decay = 0.8
second_decay = 0.9
epsilon = 1e-08
learn_rate = 0.01

SCATTER_TYPE = jnp.float32
GATHER_TYPE = jnp.float32
MESH = pl.DeviceIdType.MESH


def moments(projection, first, second):
    first_new = first_decay * first + (1.0 - first_decay) * projection
    second_new = second_decay * second + (1.0 - second_decay) * projection * projection
    normed = first_new / (jnp.sqrt(second_new) + epsilon)
    return (first_new, second_new, normed)


def contract(basis, cotangent):
    upper = basis.astype(jnp.bfloat16)
    lower = (basis - upper.astype(jnp.float32)).astype(jnp.bfloat16)
    dims = (((0,), (0,)), ((), ()))
    high_part = lax.dot_general(upper, cotangent, dims, preferred_element_type=jnp.float32)
    low_part = lax.dot_general(lower, cotangent, dims, preferred_element_type=jnp.float32)
    return high_part + low_part


class Plan:
    def __init__(self, mesh_shape, rows, rank, key_cols, value_cols):
        self.F, self.R, self.T = (mesh_shape[a] for a in ("fs", "rep", "tp"))
        self.rows, self.rank = rows, rank
        self.kc, self.vc = key_cols, value_cols
        self.cols = key_cols + value_cols
        self.piece = math.gcd(rows, 64)
        self.pieces = rows // self.piece
        self.dup = 1 if self.R == 2 and self.pieces >= 4 else 0
        self.half = self.rank // self.R
        owners = self.F
        while self.half % owners or (self.half // owners) % 16 or self.F % owners:
            owners -= 1
        self.owners = owners
        self.slice = self.half // owners


def kernel(
    plan,
    x_hbm, kcot_hbm, vcot_hbm, kfac_hbm, vfac_hbm, kw_hbm, vw_hbm, kf_hbm, ks_hbm, vf_hbm, vs_hbm,
    wall, total, squares_out,
    x, kcot, vcot, kfac, vfac, kw, vw, kf, ks, vf, vs,
    partial, ysend, yrecv, half, zsend, zrecv, sq,
    load_sem, zs_sem, zr_sem, ys_sem, yr_sem, ds_sem, dr_sem,
    rys, ryr, rzs, rzr, gzs, gzr, gys, gyr, ts, tr,
):
    F, R, T = plan.F, plan.R, plan.T
    NP, PR, C = plan.pieces, plan.piece, plan.cols
    z = lax.axis_index("fs")
    y = lax.axis_index("rep")
    t = lax.axis_index("tp")

    loads = [
        pltpu.make_async_copy(s, d, load_sem.at[i])
        for i, (s, d) in enumerate(
            (
                (x_hbm, x), (kfac_hbm, kfac), (kcot_hbm, kcot), (vfac_hbm, vfac), (vcot_hbm, vcot),
                (kw_hbm, kw), (vw_hbm, vw),
                (kf_hbm, kf), (ks_hbm, ks), (vf_hbm, vf), (vs_hbm, vs),
            )
        )
    ]
    for i in (5, 6, 0, 1, 2, 3, 4, 7, 8, 9, 10):
        loads[i].start()

    def fs_peer(j):
        return lax.rem(z + j, F)

    def rep_peer(j):
        return lax.rem(y + j, R)

    def tp_peer(j):
        return lax.rem(t + j, T)

    barrier = pltpu.get_barrier_semaphore()
    for axis, size, peer in (("fs", F, fs_peer), ("rep", R, rep_peer), ("tp", T, tp_peer)):
        for j in range(1, size):
            pl.semaphore_signal(barrier, 1, device_id={axis: peer(j)}, device_id_type=MESH)

    own = wall.at[z, y]
    for i in (5, 6):
        loads[i].wait()
    own[:, : plan.kc] = kw[...].astype(jnp.bfloat16)
    own[:, plan.kc :] = vw[...].astype(jnp.bfloat16)
    pl.semaphore_wait(barrier, F + R + T - 3)

    def rc(src, dst, s, r, axis, target):
        return pltpu.make_async_remote_copy(
            src_ref=src, dst_ref=dst, send_sem=s, recv_sem=r,
            device_id={axis: target}, device_id_type=MESH,
        )

    def prows(p):
        return pl.ds(p * PR, PR)

    def fs_copy(direction, s, p, wait=False):
        if direction == 0:
            source, target, ok = z - s, z + 1, z < F - 1
        else:
            source, target, ok = z + s, z - 1, z > 0
        source = jnp.clip(source, 0, F - 1)
        target = jnp.clip(target, 0, F - 1)
        ref = wall.at[source, y, prows(p)]
        sem = s if wait else s + 1
        return rc(ref, ref, zs_sem.at[direction, s, p], zr_sem.at[direction, sem, p], "fs", target)

    def dup_copy(direction, s, wait=False):
        if direction == 0:
            source, target = z - s, z + 1
        else:
            source, target = z + s, z - 1
        source = jnp.clip(source, 0, F - 1)
        target = jnp.clip(target, 0, F - 1)
        ref = wall.at[source, 1 - y, prows(0)]
        sem = s if wait else s + 1
        return rc(ref, ref, ds_sem.at[direction, s], dr_sem.at[direction, sem], "fs", target)

    def onward(direction):
        return z < F - 1 if direction == 0 else z > 0

    def arrives(direction, s):
        return z - s >= 0 if direction == 0 else z + s < F

    def rep_copy(source, p, j):
        ref = wall.at[source, y, prows(p)]
        return rc(ref, ref, ys_sem.at[source, p, j], yr_sem.at[source, p, j], "rep", rep_peer(j))

    def rep_arrival(source, p, j):
        ref = wall.at[source, lax.rem(y + R - j, R), prows(p)]
        return rc(ref, ref, ys_sem.at[source, p, j], yr_sem.at[source, p, j], "rep", rep_peer(j))

    def send_own(lo, hi):
        for p in range(lo, hi):
            for j in range(1, R):
                rep_copy(z, p, j).start()
            for d in (0, 1):

                @pl.when(onward(d))
                def _():
                    fs_copy(d, 0, p).start()

    def relay(s, lo, hi):
        if s >= F:
            return
        for p in range(lo, hi):
            for d in (0, 1):

                @pl.when(arrives(d, s))
                def _():
                    source = z - s if d == 0 else z + s
                    fs_copy(d, s, p, wait=True).wait_recv()
                    if s < F - 1:

                        @pl.when(onward(d))
                        def _():
                            fs_copy(d, s, p).start()

                    if not (plan.dup and p == 0):
                        for j in range(1, R):
                            rep_copy(source, p, j).start()

        if plan.dup and hi == NP:
            for d in (0, 1):

                @pl.when(arrives(d, s))
                def _():
                    dup_copy(d, s, wait=True).wait_recv()
                    if s < F - 1:

                        @pl.when(onward(d))
                        def _():
                            dup_copy(d, s).start()

    NH = (NP + 1) // 2
    send_own(0, NH)

    for i in (0, 1, 2):
        loads[i].wait()
    basis = jnp.dot(x[...], kfac[...], preferred_element_type=jnp.float32)
    partial[:, : plan.kc] = contract(basis, kcot[...])
    for i in (3, 4):
        loads[i].wait()
    basis = jnp.dot(x[...], vfac[...], preferred_element_type=jnp.float32)
    partial[:, plan.kc :] = contract(basis, vcot[...])

    H = plan.half
    ysend[...] = partial[...].astype(SCATTER_TYPE)
    for j in range(1, R):
        to = rep_peer(j)
        rc(ysend.at[pl.ds(to * H, H)], yrecv.at[j], rys.at[j], ryr.at[j], "rep", to).start()
    send_own(NH, NP)
    if plan.dup:
        rep_arrival(z, 0, 1).wait_recv()
        for d in (0, 1):

            @pl.when(onward(d))
            def _():
                dup_copy(d, 0).start()

    acc = partial[pl.ds(y * H, H), :]
    for j in range(1, R):
        rc(ysend.at[pl.ds(0, H)], yrecv.at[j], rys.at[j], ryr.at[j], "rep", rep_peer(j)).wait_recv()
        acc = acc + yrecv[j].astype(jnp.float32)
    half[...] = acc
    zsend[...] = acc.astype(SCATTER_TYPE)

    S, O = plan.slice, plan.owners

    def slice_copy(j):
        to = fs_peer(j)
        rows = pl.ds(jnp.minimum(to, O - 1) * S, S)
        return rc(zsend.at[rows], zrecv.at[j], rzs.at[j], rzr.at[j], "fs", to)

    for j in range(1, F):

        @pl.when(fs_peer(j) < O)
        def _():
            slice_copy(j).start()

    relay(1, 0, NH)

    mine = pl.ds(y * H + jnp.minimum(z, O - 1) * S, S)

    def sum_copy(j):
        return rc(total.at[mine], total.at[mine], gzs.at[j], gzr.at[j], "fs", fs_peer(j))

    @pl.when(z < O)
    def _():
        acc = half[pl.ds(jnp.minimum(z, O - 1) * S, S), :]
        for j in range(1, F):
            slice_copy(j).wait_recv()
            acc = acc + zrecv[j].astype(jnp.float32)
        total[mine, :] = acc.astype(GATHER_TYPE)
        for j in range(1, F):
            sum_copy(j).start()

    relay(1, NH, NP)

    for j in range(1, F):
        src = lax.rem(z + F - j, F)

        @pl.when(src < O)
        def _():
            rows = pl.ds(y * H + jnp.minimum(src, O - 1) * S, S)
            rc(total.at[rows], total.at[rows], gzs.at[j], gzr.at[j], "fs", fs_peer(j)).wait_recv()

    def half_copy(j):
        rows = pl.ds(y * H, H)
        return rc(total.at[rows], total.at[rows], gys.at[j], gyr.at[j], "rep", rep_peer(j))

    for j in range(1, R):
        half_copy(j).start()

    relay(2, 0, NH)

    for j in range(1, R):
        rows = pl.ds(lax.rem(y + R - j, R) * H, H)
        rc(total.at[rows], total.at[rows], gys.at[j], gyr.at[j], "rep", rep_peer(j)).wait_recv()

    for i in (7, 8, 9, 10):
        loads[i].wait()
    squares = jnp.zeros((1, 1), jnp.float32)
    for lo, hi, first, second in ((0, plan.kc, kf, ks), (plan.kc, plan.cols, vf, vs)):
        proj = total[:, lo:hi].astype(jnp.float32)
        _, _, normed = moments(proj, first[...], second[...])
        line = jnp.sum(normed * normed, axis=0, keepdims=True)
        squares = squares + jnp.sum(line, axis=1, keepdims=True)
    sq[t] = jnp.broadcast_to(squares, (8, 128))

    def sq_copy(j):
        return rc(sq.at[t], sq.at[t], ts.at[j], tr.at[j], "tp", tp_peer(j))

    for j in range(1, T):
        sq_copy(j).start()

    relay(2, NH, NP)

    for j in range(1, T):
        src = lax.rem(t + T - j, T)
        rc(sq.at[src], sq.at[src], ts.at[j], tr.at[j], "tp", tp_peer(j)).wait_recv()
    acc = sq[0]
    for i in range(1, T):
        acc = acc + sq[i]
    squares_out[...] = acc

    for s in range(3, F):
        relay(s, 0, NP)

    for source in range(F):
        for p in range(NP):
            for j in range(1, R):
                if plan.dup and p == 0:

                    @pl.when(z == source)
                    def _():
                        rep_copy(source, p, j).wait_send()
                else:
                    rep_arrival(source, p, j).wait_recv()
                    rep_copy(source, p, j).wait_send()
    for s in range(F - 1):
        for d in (0, 1):

            @pl.when(jnp.logical_and(arrives(d, s), onward(d)))
            def _():
                for p in range(NP):
                    fs_copy(d, s, p).wait_send()
                if plan.dup:
                    dup_copy(d, s).wait_send()
    for j in range(1, R):
        rc(ysend.at[pl.ds(0, H)], yrecv.at[j], rys.at[j], ryr.at[j], "rep", rep_peer(j)).wait_send()
        half_copy(j).wait_send()
    for j in range(1, F):

        @pl.when(fs_peer(j) < O)
        def _():
            slice_copy(j).wait_send()

        @pl.when(z < O)
        def _():
            sum_copy(j).wait_send()
    for j in range(1, T):
        sq_copy(j).wait_send()


def exchange(plan, *args):
    F, R, T, NP, C = plan.F, plan.R, plan.T, plan.pieces, plan.cols
    f32 = jnp.float32
    vmem = pl.BlockSpec(memory_space=pltpu.VMEM)
    hbm = pl.BlockSpec(memory_space=pltpu.HBM)
    dma = pltpu.SemaphoreType.DMA
    rank = plan.rank
    out_shape = (
        jax.ShapeDtypeStruct((F, R, plan.rows, C), jnp.bfloat16),
        jax.ShapeDtypeStruct((rank, C), GATHER_TYPE),
        jax.ShapeDtypeStruct((8, 128), f32),
    )
    scratch = [pltpu.VMEM(a.shape, a.dtype) for a in args]
    scratch += [
        pltpu.VMEM((rank, C), f32),
        pltpu.VMEM((rank, C), SCATTER_TYPE),
        pltpu.VMEM((R, plan.half, C), SCATTER_TYPE),
        pltpu.VMEM((plan.half, C), f32),
        pltpu.VMEM((plan.half, C), SCATTER_TYPE),
        pltpu.VMEM((F, plan.slice, C), SCATTER_TYPE),
        pltpu.VMEM((T, 8, 128), f32),
        dma((11,)),
        dma((2, F, NP)),
        dma((2, F, NP)),
        dma((F, NP, R)),
        dma((F, NP, R)),
        dma((2, F)),
        dma((2, F)),
        dma((R,)), dma((R,)),
        dma((F,)), dma((F,)),
        dma((F,)), dma((F,)),
        dma((R,)), dma((R,)),
        dma((T,)), dma((T,)),
    ]
    return pl.pallas_call(
        functools.partial(kernel, plan),
        out_shape=out_shape,
        in_specs=[hbm] * 11,
        out_specs=[vmem] * 3,
        scratch_shapes=scratch,
        compiler_params=pltpu.CompilerParams(
            collective_id=0, has_side_effects=True, vmem_limit_bytes=28 * 1024 * 1024
        ),
    )(*args)


BLOCKS = 8


def finish(
    plan, kfac, vfac, kw, vw, kf, ks, vf, vs, wall, total, squares,
    kw_out, vw_out, kf_out, ks_out, vf_out, vs_out, kstep_out, vstep_out, kcopy_out, vcopy_out,
    kw_new, vw_new, kf_new, ks_new, vf_new, vs_new, kstep, vstep, kcopy, vcopy, sem, copy_sem,
):
    me = lax.axis_index("fs") * plan.R + lax.axis_index("rep")
    mine = pl.ds(me * plan.rows, plan.rows)
    entries = jnp.float32(plan.rank * plan.cols * plan.T)
    shrink = jnp.sqrt(entries / (entries + squares[0:1, 0:1]))
    depth = kfac.shape[0] // BLOCKS

    def out(i, src, dst):
        c = pltpu.make_async_copy(src, dst, sem.at[i])
        c.start()
        return c

    sides = (
        (0, plan.kc, kfac, kw, kf, ks, (kf_new, ks_new, kstep, kw_new), (kf_out, ks_out, kstep_out, kw_out)),
        (plan.kc, plan.cols, vfac, vw, vf, vs, (vf_new, vs_new, vstep, vw_new), (vf_out, vs_out, vstep_out, vw_out)),
    )
    pending, uppers, lowers = [], [], []
    for k, (lo, hi, _, _, first, second, news, outs) in enumerate(sides):
        proj = total[:, lo:hi].astype(jnp.float32)
        first_new, second_new, normed = moments(proj, first[...], second[...])
        news[0][...] = first_new
        news[1][...] = second_new
        upper = normed.astype(jnp.bfloat16)
        uppers.append(upper)
        lowers.append((normed - upper.astype(jnp.float32)).astype(jnp.bfloat16))
        for i in (0, 1):
            pending.append(out(4 * k + i, news[i], outs[i]))

    for b in range(BLOCKS):
        rows = pl.ds(b * depth, depth)
        for k, (dst, dst_out) in enumerate(((kcopy, kcopy_out), (vcopy, vcopy_out))):
            lo, hi, factor = sides[k][:3]
            full = jnp.dot(factor[rows, :], uppers[k], preferred_element_type=jnp.float32)
            step = shrink * full
            dst[rows, :] = (wall[rows, lo:hi].astype(jnp.float32) - learn_rate * step).astype(
                jnp.bfloat16
            )
            c = pltpu.make_async_copy(dst.at[rows], dst_out.at[rows], copy_sem.at[k, b])
            c.start()
            pending.append(c)

    for k, (lo, hi, factor, weight, _, _, news, outs) in enumerate(sides):
        part = factor[mine, :]
        step = jnp.dot(part, uppers[k], preferred_element_type=jnp.float32)
        step = shrink * (step + jnp.dot(part, lowers[k], preferred_element_type=jnp.float32))
        news[2][...] = step
        news[3][...] = weight[...] - learn_rate * step
        for i in (2, 3):
            pending.append(out(4 * k + i, news[i], outs[i]))
    for c in pending:
        c.wait()


def body(mesh_shape, *args):
    (x, kcot, vcot, kfac, vfac, kw, vw, kf, ks, vf, vs) = args
    rows, key_cols = kw.shape
    value_cols = vw.shape[1]
    plan = Plan(mesh_shape, rows, kf.shape[0], key_cols, value_cols)
    wall, total, squares = exchange(plan, *args)
    wall = wall.reshape(-1, plan.cols)
    like = [jax.ShapeDtypeStruct(a.shape, a.dtype) for a in (kw, vw, kf, ks, vf, vs, kw, vw)]
    depth = kfac.shape[0]
    like += [jax.ShapeDtypeStruct((depth, c), jnp.bfloat16) for c in (key_cols, value_cols)]
    vmem = pl.BlockSpec(memory_space=pltpu.VMEM)
    return pl.pallas_call(
        functools.partial(finish, plan),
        out_shape=like,
        in_specs=[vmem] * 11,
        out_specs=[pl.BlockSpec(memory_space=pl.ANY)] * 10,
        scratch_shapes=[pltpu.VMEM(a.shape, a.dtype) for a in like]
        + [pltpu.SemaphoreType.DMA((8,)), pltpu.SemaphoreType.DMA((2, BLOCKS))],
        compiler_params=pltpu.CompilerParams(vmem_limit_bytes=20 * 1024 * 1024),
    )(kfac, vfac, kw, vw, kf, ks, vf, vs, wall, total, squares)


def solution(mesh):
    rows = P(("fs", "rep"), "tp")
    cols = P(None, "tp")
    in_specs = (P(("fs", "rep"), None), rows, rows, P(), P(), rows, rows, cols, cols, cols, cols)
    out_specs = (rows, rows, cols, cols, cols, cols, rows, rows, cols, cols)
    return jax.shard_map(
        functools.partial(body, dict(mesh.shape)),
        mesh=mesh, in_specs=in_specs, out_specs=out_specs, check_vma=False,
    )
```

```python
import functools
import math

import jax
import jax.numpy as jnp
from jax import lax
from jax.experimental import pallas as pl
from jax.experimental.pallas import tpu as pltpu
from jax.sharding import PartitionSpec as P

first_decay = 0.8
second_decay = 0.9
epsilon = 1e-08
learn_rate = 0.01

REP_TYPE = jnp.bfloat16
FS_TYPE = jnp.float32
GATHER_TYPE = jnp.bfloat16
MESH = pl.DeviceIdType.MESH


def moments(projection, first, second):
    first_new = first_decay * first + (1.0 - first_decay) * projection
    second_new = second_decay * second + (1.0 - second_decay) * projection * projection
    normed = first_new / (jnp.sqrt(second_new) + epsilon)
    return (first_new, second_new, normed)


def contract(basis, cotangent):
    upper = basis.astype(jnp.bfloat16)
    lower = (basis - upper.astype(jnp.float32)).astype(jnp.bfloat16)
    dims = (((0,), (0,)), ((), ()))
    high_part = lax.dot_general(upper, cotangent, dims, preferred_element_type=jnp.float32)
    low_part = lax.dot_general(lower, cotangent, dims, preferred_element_type=jnp.float32)
    return high_part + low_part


class Plan:
    def __init__(self, mesh_shape, rows, rank, key_cols, value_cols):
        self.F, self.R, self.T = (mesh_shape[a] for a in ("fs", "rep", "tp"))
        self.rows, self.rank = rows, rank
        self.kc, self.vc = key_cols, value_cols
        self.cols = key_cols + value_cols
        self.piece = math.gcd(rows, 64)
        self.pieces = rows // self.piece
        self.dup = 1 if self.R == 2 and self.pieces >= 4 else 0
        self.half = self.rank // self.R
        owners = self.F
        while self.half % owners or (self.half // owners) % 16 or self.F % owners:
            owners -= 1
        self.owners = owners
        self.slice = self.half // owners


def kernel(
    plan,
    x_hbm, kcot_hbm, vcot_hbm, kfac_hbm, vfac_hbm, kw_hbm, vw_hbm, kf_hbm, ks_hbm, vf_hbm, vs_hbm,
    wall, total, squares_out, kfac, vfac, kw, vw, kf, ks, vf, vs,
    x, kcot, vcot,
    partial, ysend, yrecv, half, zsend, zrecv, sq,
    load_sem, zs_sem, zr_sem, ys_sem, yr_sem, ds_sem, dr_sem,
    rys, ryr, rzs, rzr, gzs, gzr, gys, gyr, ts, tr,
):
    F, R, T = plan.F, plan.R, plan.T
    NP, PR, C = plan.pieces, plan.piece, plan.cols
    z = lax.axis_index("fs")
    y = lax.axis_index("rep")
    t = lax.axis_index("tp")

    loads = [
        pltpu.make_async_copy(s, d, load_sem.at[i])
        for i, (s, d) in enumerate(
            (
                (x_hbm, x), (kfac_hbm, kfac), (kcot_hbm, kcot), (vfac_hbm, vfac), (vcot_hbm, vcot),
                (kw_hbm, kw), (vw_hbm, vw),
                (kf_hbm, kf), (ks_hbm, ks), (vf_hbm, vf), (vs_hbm, vs),
            )
        )
    ]
    for i in (5, 6, 0, 1, 2, 3, 4, 7, 8, 9, 10):
        loads[i].start()

    def fs_peer(j):
        return lax.rem(z + j, F)

    def rep_peer(j):
        return lax.rem(y + j, R)

    def tp_peer(j):
        return lax.rem(t + j, T)

    barrier = pltpu.get_barrier_semaphore()
    for axis, size, peer in (("fs", F, fs_peer), ("rep", R, rep_peer), ("tp", T, tp_peer)):
        for j in range(1, size):
            pl.semaphore_signal(barrier, 1, device_id={axis: peer(j)}, device_id_type=MESH)

    own = wall.at[z, y]
    for i in (5, 6):
        loads[i].wait()
    own[:, : plan.kc] = kw[...].astype(jnp.bfloat16)
    own[:, plan.kc :] = vw[...].astype(jnp.bfloat16)
    pl.semaphore_wait(barrier, F + R + T - 3)

    def rc(src, dst, s, r, axis, target):
        return pltpu.make_async_remote_copy(
            src_ref=src, dst_ref=dst, send_sem=s, recv_sem=r,
            device_id={axis: target}, device_id_type=MESH,
        )

    def prows(p):
        return pl.ds(p * PR, PR)

    def fs_copy(direction, s, p, wait=False):
        if direction == 0:
            source, target, ok = z - s, z + 1, z < F - 1
        else:
            source, target, ok = z + s, z - 1, z > 0
        source = jnp.clip(source, 0, F - 1)
        target = jnp.clip(target, 0, F - 1)
        ref = wall.at[source, y, prows(p)]
        sem = s if wait else s + 1
        return rc(ref, ref, zs_sem.at[direction, s, p], zr_sem.at[direction, sem, p], "fs", target)

    def dup_copy(direction, s, wait=False):
        if direction == 0:
            source, target = z - s, z + 1
        else:
            source, target = z + s, z - 1
        source = jnp.clip(source, 0, F - 1)
        target = jnp.clip(target, 0, F - 1)
        ref = wall.at[source, 1 - y, prows(0)]
        sem = s if wait else s + 1
        return rc(ref, ref, ds_sem.at[direction, s], dr_sem.at[direction, sem], "fs", target)

    def onward(direction):
        return z < F - 1 if direction == 0 else z > 0

    def arrives(direction, s):
        return z - s >= 0 if direction == 0 else z + s < F

    def rep_copy(source, p, j):
        ref = wall.at[source, y, prows(p)]
        return rc(ref, ref, ys_sem.at[source, p, j], yr_sem.at[source, p, j], "rep", rep_peer(j))

    def rep_arrival(source, p, j):
        ref = wall.at[source, lax.rem(y + R - j, R), prows(p)]
        return rc(ref, ref, ys_sem.at[source, p, j], yr_sem.at[source, p, j], "rep", rep_peer(j))

    def send_own(lo, hi):
        for p in range(lo, hi):
            for j in range(1, R):
                rep_copy(z, p, j).start()
            for d in (0, 1):

                @pl.when(onward(d))
                def _():
                    fs_copy(d, 0, p).start()

    def relay(s, lo, hi):
        if s >= F:
            return
        for p in range(lo, hi):
            for d in (0, 1):

                @pl.when(arrives(d, s))
                def _():
                    source = z - s if d == 0 else z + s
                    fs_copy(d, s, p, wait=True).wait_recv()
                    if s < F - 1:

                        @pl.when(onward(d))
                        def _():
                            fs_copy(d, s, p).start()

                    if not (plan.dup and p == 0):
                        for j in range(1, R):
                            rep_copy(source, p, j).start()

        if plan.dup and hi == NP:
            for d in (0, 1):

                @pl.when(arrives(d, s))
                def _():
                    dup_copy(d, s, wait=True).wait_recv()
                    if s < F - 1:

                        @pl.when(onward(d))
                        def _():
                            dup_copy(d, s).start()

    NH = (NP + 1) // 2
    send_own(0, NH)

    for i in (0, 1, 2):
        loads[i].wait()
    basis = jnp.dot(x[...], kfac[...], preferred_element_type=jnp.float32)
    partial[:, : plan.kc] = contract(basis, kcot[...])
    for i in (3, 4):
        loads[i].wait()
    basis = jnp.dot(x[...], vfac[...], preferred_element_type=jnp.float32)
    partial[:, plan.kc :] = contract(basis, vcot[...])

    H = plan.half
    ysend[...] = partial[...].astype(REP_TYPE)
    for j in range(1, R):
        to = rep_peer(j)
        rc(ysend.at[pl.ds(to * H, H)], yrecv.at[j], rys.at[j], ryr.at[j], "rep", to).start()
    send_own(NH, NP)
    if plan.dup:
        rep_arrival(z, 0, 1).wait_recv()
        for d in (0, 1):

            @pl.when(onward(d))
            def _():
                dup_copy(d, 0).start()

    acc = partial[pl.ds(y * H, H), :]
    for j in range(1, R):
        rc(ysend.at[pl.ds(0, H)], yrecv.at[j], rys.at[j], ryr.at[j], "rep", rep_peer(j)).wait_recv()
        acc = acc + yrecv[j].astype(jnp.float32)
    half[...] = acc
    zsend[...] = acc.astype(FS_TYPE)

    S, O = plan.slice, plan.owners

    def slice_copy(j):
        to = fs_peer(j)
        rows = pl.ds(jnp.minimum(to, O - 1) * S, S)
        return rc(zsend.at[rows], zrecv.at[j], rzs.at[j], rzr.at[j], "fs", to)

    for j in range(1, F):

        @pl.when(fs_peer(j) < O)
        def _():
            slice_copy(j).start()

    relay(1, 0, NH)

    mine = pl.ds(y * H + jnp.minimum(z, O - 1) * S, S)

    def sum_copy(j):
        return rc(total.at[mine], total.at[mine], gzs.at[j], gzr.at[j], "fs", fs_peer(j))

    @pl.when(z < O)
    def _():
        acc = half[pl.ds(jnp.minimum(z, O - 1) * S, S), :]
        for j in range(1, F):
            slice_copy(j).wait_recv()
            acc = acc + zrecv[j].astype(jnp.float32)
        total[mine, :] = acc.astype(GATHER_TYPE)
        for j in range(1, F):
            sum_copy(j).start()

    relay(1, NH, NP)

    for j in range(1, F):
        src = lax.rem(z + F - j, F)

        @pl.when(src < O)
        def _():
            rows = pl.ds(y * H + jnp.minimum(src, O - 1) * S, S)
            rc(total.at[rows], total.at[rows], gzs.at[j], gzr.at[j], "fs", fs_peer(j)).wait_recv()

    def half_copy(j):
        rows = pl.ds(y * H, H)
        return rc(total.at[rows], total.at[rows], gys.at[j], gyr.at[j], "rep", rep_peer(j))

    for j in range(1, R):
        half_copy(j).start()

    for s in range(2, F):
        relay(s, 0, NP)

    for j in range(1, R):
        rows = pl.ds(lax.rem(y + R - j, R) * H, H)
        rc(total.at[rows], total.at[rows], gys.at[j], gyr.at[j], "rep", rep_peer(j)).wait_recv()

    for i in (7, 8, 9, 10):
        loads[i].wait()
    squares = jnp.zeros((1, 1), jnp.float32)
    for lo, hi, first, second in ((0, plan.kc, kf, ks), (plan.kc, plan.cols, vf, vs)):
        proj = total[:, lo:hi].astype(jnp.float32)
        _, _, normed = moments(proj, first[...], second[...])
        line = jnp.sum(normed * normed, axis=0, keepdims=True)
        squares = squares + jnp.sum(line, axis=1, keepdims=True)
    sq[t] = jnp.broadcast_to(squares, (8, 128))

    def sq_copy(j):
        return rc(sq.at[t], sq.at[t], ts.at[j], tr.at[j], "tp", tp_peer(j))

    for j in range(1, T):
        sq_copy(j).start()

    for j in range(1, T):
        src = lax.rem(t + T - j, T)
        rc(sq.at[src], sq.at[src], ts.at[j], tr.at[j], "tp", tp_peer(j)).wait_recv()
    acc = sq[0]
    for i in range(1, T):
        acc = acc + sq[i]
    squares_out[...] = acc

    for source in range(F):
        for p in range(NP):
            for j in range(1, R):
                if plan.dup and p == 0:

                    @pl.when(z == source)
                    def _():
                        rep_copy(source, p, j).wait_send()
                else:
                    rep_arrival(source, p, j).wait_recv()
                    rep_copy(source, p, j).wait_send()
    for s in range(F - 1):
        for d in (0, 1):

            @pl.when(jnp.logical_and(arrives(d, s), onward(d)))
            def _():
                for p in range(NP):
                    fs_copy(d, s, p).wait_send()
                if plan.dup:
                    dup_copy(d, s).wait_send()
    for j in range(1, R):
        rc(ysend.at[pl.ds(0, H)], yrecv.at[j], rys.at[j], ryr.at[j], "rep", rep_peer(j)).wait_send()
        half_copy(j).wait_send()
    for j in range(1, F):

        @pl.when(fs_peer(j) < O)
        def _():
            slice_copy(j).wait_send()

        @pl.when(z < O)
        def _():
            sum_copy(j).wait_send()
    for j in range(1, T):
        sq_copy(j).wait_send()


def exchange(plan, *args):
    F, R, T, NP, C = plan.F, plan.R, plan.T, plan.pieces, plan.cols
    f32 = jnp.float32
    vmem = pl.BlockSpec(memory_space=pltpu.VMEM)
    hbm = pl.BlockSpec(memory_space=pltpu.HBM)
    dma = pltpu.SemaphoreType.DMA
    rank = plan.rank
    out_shape = (
        jax.ShapeDtypeStruct((F, R, plan.rows, C), jnp.bfloat16),
        jax.ShapeDtypeStruct((rank, C), GATHER_TYPE),
        jax.ShapeDtypeStruct((8, 128), f32),
    ) + tuple(jax.ShapeDtypeStruct(a.shape, a.dtype) for a in args[3:])
    scratch = [pltpu.VMEM(a.shape, a.dtype) for a in args[:3]]
    scratch += [
        pltpu.VMEM((rank, C), f32),
        pltpu.VMEM((rank, C), REP_TYPE),
        pltpu.VMEM((R, plan.half, C), REP_TYPE),
        pltpu.VMEM((plan.half, C), f32),
        pltpu.VMEM((plan.half, C), FS_TYPE),
        pltpu.VMEM((F, plan.slice, C), FS_TYPE),
        pltpu.VMEM((T, 8, 128), f32),
        dma((11,)),
        dma((2, F, NP)),
        dma((2, F, NP)),
        dma((F, NP, R)),
        dma((F, NP, R)),
        dma((2, F)),
        dma((2, F)),
        dma((R,)), dma((R,)),
        dma((F,)), dma((F,)),
        dma((F,)), dma((F,)),
        dma((R,)), dma((R,)),
        dma((T,)), dma((T,)),
    ]
    return pl.pallas_call(
        functools.partial(kernel, plan),
        out_shape=out_shape,
        in_specs=[hbm] * 11,
        out_specs=[vmem] * 11,
        scratch_shapes=scratch,
        compiler_params=pltpu.CompilerParams(
            collective_id=0, has_side_effects=True, vmem_limit_bytes=40 * 1024 * 1024
        ),
    )(*(pltpu.with_memory_space_constraint(a, pltpu.HBM) for a in args))


BLOCKS = 8


def finish(
    plan, kfac, vfac, kw, vw, kf, ks, vf, vs, wall, total, squares,
    kw_out, vw_out, kf_out, ks_out, vf_out, vs_out, kstep_out, vstep_out, kcopy_out, vcopy_out,
    kw_new, vw_new, kf_new, ks_new, vf_new, vs_new, kstep, vstep, kcopy, vcopy, sem, copy_sem,
):
    me = lax.axis_index("fs") * plan.R + lax.axis_index("rep")
    mine = pl.ds(me * plan.rows, plan.rows)
    entries = jnp.float32(plan.rank * plan.cols * plan.T)
    shrink = jnp.sqrt(entries / (entries + squares[0:1, 0:1]))
    depth = kfac.shape[0] // BLOCKS

    def out(i, src, dst):
        c = pltpu.make_async_copy(src, dst, sem.at[i])
        c.start()
        return c

    sides = (
        (0, plan.kc, kfac, kw, kf, ks, (kf_new, ks_new, kstep, kw_new), (kf_out, ks_out, kstep_out, kw_out)),
        (plan.kc, plan.cols, vfac, vw, vf, vs, (vf_new, vs_new, vstep, vw_new), (vf_out, vs_out, vstep_out, vw_out)),
    )
    pending, uppers, lowers = [], [], []
    for k, (lo, hi, _, _, first, second, news, outs) in enumerate(sides):
        proj = total[:, lo:hi].astype(jnp.float32)
        first_new, second_new, normed = moments(proj, first[...], second[...])
        news[0][...] = first_new
        news[1][...] = second_new
        upper = normed.astype(jnp.bfloat16)
        uppers.append(upper)
        lowers.append((normed - upper.astype(jnp.float32)).astype(jnp.bfloat16))
        for i in (0, 1):
            pending.append(out(4 * k + i, news[i], outs[i]))

    for b in range(BLOCKS):
        rows = pl.ds(b * depth, depth)
        for k, (dst, dst_out) in enumerate(((kcopy, kcopy_out), (vcopy, vcopy_out))):
            lo, hi, factor = sides[k][:3]
            full = jnp.dot(factor[rows, :], uppers[k], preferred_element_type=jnp.float32)
            step = shrink * full
            dst[rows, :] = (wall[rows, lo:hi].astype(jnp.float32) - learn_rate * step).astype(
                jnp.bfloat16
            )
            c = pltpu.make_async_copy(dst.at[rows], dst_out.at[rows], copy_sem.at[k, b])
            c.start()
            pending.append(c)

    for k, (lo, hi, factor, weight, _, _, news, outs) in enumerate(sides):
        part = factor[mine, :]
        step = jnp.dot(part, uppers[k], preferred_element_type=jnp.float32)
        step = shrink * (step + jnp.dot(part, lowers[k], preferred_element_type=jnp.float32))
        news[2][...] = step
        news[3][...] = weight[...] - learn_rate * step
        for i in (2, 3):
            pending.append(out(4 * k + i, news[i], outs[i]))
    for c in pending:
        c.wait()


def body(mesh_shape, *args):
    (x, kcot, vcot, kfac, vfac, kw, vw, kf, ks, vf, vs) = args
    rows, key_cols = kw.shape
    value_cols = vw.shape[1]
    plan = Plan(mesh_shape, rows, kf.shape[0], key_cols, value_cols)
    wall, total, squares, *held = exchange(plan, *args)
    wall = wall.reshape(-1, plan.cols)
    like = [jax.ShapeDtypeStruct(a.shape, a.dtype) for a in (kw, vw, kf, ks, vf, vs, kw, vw)]
    depth = kfac.shape[0]
    like += [jax.ShapeDtypeStruct((depth, c), jnp.bfloat16) for c in (key_cols, value_cols)]
    vmem = pl.BlockSpec(memory_space=pltpu.VMEM)
    return pl.pallas_call(
        functools.partial(finish, plan),
        out_shape=like,
        in_specs=[vmem] * 11,
        out_specs=[pl.BlockSpec(memory_space=pl.ANY)] * 10,
        scratch_shapes=[pltpu.VMEM(a.shape, a.dtype) for a in like]
        + [pltpu.SemaphoreType.DMA((8,)), pltpu.SemaphoreType.DMA((2, BLOCKS))],
        compiler_params=pltpu.CompilerParams(vmem_limit_bytes=20 * 1024 * 1024),
    )(*held, wall, total, squares)


def solution(mesh):
    rows = P(("fs", "rep"), "tp")
    cols = P(None, "tp")
    in_specs = (P(("fs", "rep"), None), rows, rows, P(), P(), rows, rows, cols, cols, cols, cols)
    out_specs = (rows, rows, cols, cols, cols, cols, rows, rows, cols, cols)
    return jax.shard_map(
        functools.partial(body, dict(mesh.shape)),
        mesh=mesh, in_specs=in_specs, out_specs=out_specs, check_vma=False,
    )
```

```python
import functools
import math

import jax
import jax.numpy as jnp
from jax import lax
from jax.experimental import pallas as pl
from jax.experimental.pallas import tpu as pltpu
from jax.sharding import PartitionSpec as P

first_decay = 0.8
second_decay = 0.9
epsilon = 1e-08
learn_rate = 0.01

REP_TYPE = jnp.bfloat16
FS_TYPE = jnp.float32
GATHER_TYPE = jnp.bfloat16
MESH = pl.DeviceIdType.MESH


def moments(projection, first, second):
    first_new = first_decay * first + (1.0 - first_decay) * projection
    second_new = second_decay * second + (1.0 - second_decay) * projection * projection
    normed = first_new / (jnp.sqrt(second_new) + epsilon)
    return (first_new, second_new, normed)


def contract(basis, cotangent):
    upper = basis.astype(jnp.bfloat16)
    lower = (basis - upper.astype(jnp.float32)).astype(jnp.bfloat16)
    dims = (((0,), (0,)), ((), ()))
    high_part = lax.dot_general(upper, cotangent, dims, preferred_element_type=jnp.float32)
    low_part = lax.dot_general(lower, cotangent, dims, preferred_element_type=jnp.float32)
    return high_part + low_part


class Plan:
    def __init__(self, mesh_shape, rows, rank, key_cols, value_cols):
        self.F, self.R, self.T = (mesh_shape[a] for a in ("fs", "rep", "tp"))
        self.rows, self.rank = rows, rank
        self.kc, self.vc = key_cols, value_cols
        self.cols = key_cols + value_cols
        self.piece = math.gcd(rows, 64)
        self.pieces = rows // self.piece
        self.dup = 1 if self.R == 2 and self.pieces >= 4 else 0
        self.half = self.rank // self.R
        owners = self.F
        while self.half % owners or (self.half // owners) % 16 or self.F % owners:
            owners -= 1
        self.owners = owners
        self.slice = self.half // owners


def kernel(
    plan,
    x_hbm, kcot_hbm, vcot_hbm, kfac_hbm, vfac_hbm, kw_hbm, vw_hbm, kf_hbm, ks_hbm, vf_hbm, vs_hbm,
    wall, total, squares_out, kfac, vfac, kw, vw, kf, ks, vf, vs,
    x, kcot, vcot,
    partial, ysend, yrecv, half, zsend, zrecv, sq,
    load_sem, zs_sem, zr_sem, ys_sem, yr_sem, ds_sem, dr_sem,
    rys, ryr, rzs, rzr, gzs, gzr, gys, gyr, ts, tr,
):
    F, R, T = plan.F, plan.R, plan.T
    NP, PR, C = plan.pieces, plan.piece, plan.cols
    z = lax.axis_index("fs")
    y = lax.axis_index("rep")
    t = lax.axis_index("tp")

    loads = [
        pltpu.make_async_copy(s, d, load_sem.at[i])
        for i, (s, d) in enumerate(
            (
                (x_hbm, x), (kfac_hbm, kfac), (kcot_hbm, kcot), (vfac_hbm, vfac), (vcot_hbm, vcot),
                (kw_hbm, kw), (vw_hbm, vw),
                (kf_hbm, kf), (ks_hbm, ks), (vf_hbm, vf), (vs_hbm, vs),
            )
        )
    ]
    for i in (5, 6, 0, 1, 2, 3, 4, 7, 8, 9, 10):
        loads[i].start()

    def fs_peer(j):
        return lax.rem(z + j, F)

    def rep_peer(j):
        return lax.rem(y + j, R)

    def tp_peer(j):
        return lax.rem(t + j, T)

    barrier = pltpu.get_barrier_semaphore()
    for axis, size, peer in (("fs", F, fs_peer), ("rep", R, rep_peer), ("tp", T, tp_peer)):
        for j in range(1, size):
            pl.semaphore_signal(barrier, 1, device_id={axis: peer(j)}, device_id_type=MESH)

    own = wall.at[z, y]
    for i in (5, 6):
        loads[i].wait()
    own[:, : plan.kc] = kw[...].astype(jnp.bfloat16)
    own[:, plan.kc :] = vw[...].astype(jnp.bfloat16)
    pl.semaphore_wait(barrier, F + R + T - 3)

    def rc(src, dst, s, r, axis, target):
        return pltpu.make_async_remote_copy(
            src_ref=src, dst_ref=dst, send_sem=s, recv_sem=r,
            device_id={axis: target}, device_id_type=MESH,
        )

    def prows(p):
        return pl.ds(p * PR, PR)

    def fs_copy(direction, s, p, wait=False):
        if direction == 0:
            source, target, ok = z - s, z + 1, z < F - 1
        else:
            source, target, ok = z + s, z - 1, z > 0
        source = jnp.clip(source, 0, F - 1)
        target = jnp.clip(target, 0, F - 1)
        ref = wall.at[source, y, prows(p)]
        sem = s if wait else s + 1
        return rc(ref, ref, zs_sem.at[direction, s, p], zr_sem.at[direction, sem, p], "fs", target)

    def dup_copy(direction, s, wait=False):
        if direction == 0:
            source, target = z - s, z + 1
        else:
            source, target = z + s, z - 1
        source = jnp.clip(source, 0, F - 1)
        target = jnp.clip(target, 0, F - 1)
        ref = wall.at[source, 1 - y, prows(0)]
        sem = s if wait else s + 1
        return rc(ref, ref, ds_sem.at[direction, s], dr_sem.at[direction, sem], "fs", target)

    def onward(direction):
        return z < F - 1 if direction == 0 else z > 0

    def arrives(direction, s):
        return z - s >= 0 if direction == 0 else z + s < F

    def rep_copy(source, p, j):
        ref = wall.at[source, y, prows(p)]
        return rc(ref, ref, ys_sem.at[source, p, j], yr_sem.at[source, p, j], "rep", rep_peer(j))

    def rep_arrival(source, p, j):
        ref = wall.at[source, lax.rem(y + R - j, R), prows(p)]
        return rc(ref, ref, ys_sem.at[source, p, j], yr_sem.at[source, p, j], "rep", rep_peer(j))

    def send_own(lo, hi):
        for p in range(lo, hi):
            for j in range(1, R):
                rep_copy(z, p, j).start()
            for d in (0, 1):

                @pl.when(onward(d))
                def _():
                    fs_copy(d, 0, p).start()

    def relay(s, lo, hi):
        if s >= F:
            return
        for p in range(lo, hi):
            for d in (0, 1):

                @pl.when(arrives(d, s))
                def _():
                    source = z - s if d == 0 else z + s
                    fs_copy(d, s, p, wait=True).wait_recv()
                    if s < F - 1:

                        @pl.when(onward(d))
                        def _():
                            fs_copy(d, s, p).start()

                    if not (plan.dup and p == 0):
                        for j in range(1, R):
                            rep_copy(source, p, j).start()

        if plan.dup and hi == NP:
            for d in (0, 1):

                @pl.when(arrives(d, s))
                def _():
                    dup_copy(d, s, wait=True).wait_recv()
                    if s < F - 1:

                        @pl.when(onward(d))
                        def _():
                            dup_copy(d, s).start()

    NH = (NP + 1) // 2
    send_own(0, NH)

    for i in (0, 1, 2):
        loads[i].wait()
    basis = jnp.dot(x[...], kfac[...], preferred_element_type=jnp.float32)
    partial[:, : plan.kc] = contract(basis, kcot[...])
    for i in (3, 4):
        loads[i].wait()
    basis = jnp.dot(x[...], vfac[...], preferred_element_type=jnp.float32)
    partial[:, plan.kc :] = contract(basis, vcot[...])

    H = plan.half
    ysend[...] = partial[...].astype(REP_TYPE)
    for j in range(1, R):
        to = rep_peer(j)
        rc(ysend.at[pl.ds(to * H, H)], yrecv.at[j], rys.at[j], ryr.at[j], "rep", to).start()
    send_own(NH, NP)
    if plan.dup:
        rep_arrival(z, 0, 1).wait_recv()
        for d in (0, 1):

            @pl.when(onward(d))
            def _():
                dup_copy(d, 0).start()

    acc = partial[pl.ds(y * H, H), :]
    for j in range(1, R):
        rc(ysend.at[pl.ds(0, H)], yrecv.at[j], rys.at[j], ryr.at[j], "rep", rep_peer(j)).wait_recv()
        acc = acc + yrecv[j].astype(jnp.float32)
    half[...] = acc
    zsend[...] = acc.astype(FS_TYPE)

    S, O = plan.slice, plan.owners

    def slice_copy(j):
        to = fs_peer(j)
        rows = pl.ds(jnp.minimum(to, O - 1) * S, S)
        return rc(zsend.at[rows], zrecv.at[j], rzs.at[j], rzr.at[j], "fs", to)

    for j in range(1, F):

        @pl.when(fs_peer(j) < O)
        def _():
            slice_copy(j).start()

    relay(1, 0, NH)

    mine = pl.ds(y * H + jnp.minimum(z, O - 1) * S, S)

    def sum_copy(j):
        return rc(total.at[mine], total.at[mine], gzs.at[j], gzr.at[j], "fs", fs_peer(j))

    @pl.when(z < O)
    def _():
        acc = half[pl.ds(jnp.minimum(z, O - 1) * S, S), :]
        for j in range(1, F):
            slice_copy(j).wait_recv()
            acc = acc + zrecv[j].astype(jnp.float32)
        total[mine, :] = acc.astype(GATHER_TYPE)
        for j in range(1, F):
            sum_copy(j).start()

    relay(1, NH, NP)

    relay(2, 0, NH)
    for j in range(1, F):
        src = lax.rem(z + F - j, F)

        @pl.when(src < O)
        def _():
            rows = pl.ds(y * H + jnp.minimum(src, O - 1) * S, S)
            rc(total.at[rows], total.at[rows], gzs.at[j], gzr.at[j], "fs", fs_peer(j)).wait_recv()

    def half_copy(j):
        rows = pl.ds(y * H, H)
        return rc(total.at[rows], total.at[rows], gys.at[j], gyr.at[j], "rep", rep_peer(j))

    for j in range(1, R):
        half_copy(j).start()

    relay(2, NH, NP)
    for s in range(3, F):
        relay(s, 0, NP)

    for j in range(1, R):
        rows = pl.ds(lax.rem(y + R - j, R) * H, H)
        rc(total.at[rows], total.at[rows], gys.at[j], gyr.at[j], "rep", rep_peer(j)).wait_recv()

    for i in (7, 8, 9, 10):
        loads[i].wait()
    squares = jnp.zeros((1, 1), jnp.float32)
    for lo, hi, first, second in ((0, plan.kc, kf, ks), (plan.kc, plan.cols, vf, vs)):
        proj = total[:, lo:hi].astype(jnp.float32)
        _, _, normed = moments(proj, first[...], second[...])
        line = jnp.sum(normed * normed, axis=0, keepdims=True)
        squares = squares + jnp.sum(line, axis=1, keepdims=True)
    sq[t] = jnp.broadcast_to(squares, (8, 128))

    def sq_copy(j):
        return rc(sq.at[t], sq.at[t], ts.at[j], tr.at[j], "tp", tp_peer(j))

    for j in range(1, T):
        sq_copy(j).start()

    for j in range(1, T):
        src = lax.rem(t + T - j, T)
        rc(sq.at[src], sq.at[src], ts.at[j], tr.at[j], "tp", tp_peer(j)).wait_recv()
    acc = sq[0]
    for i in range(1, T):
        acc = acc + sq[i]
    squares_out[...] = acc

    for source in range(F):
        for p in range(NP):
            for j in range(1, R):
                if plan.dup and p == 0:

                    @pl.when(z == source)
                    def _():
                        rep_copy(source, p, j).wait_send()
                else:
                    rep_arrival(source, p, j).wait_recv()
                    rep_copy(source, p, j).wait_send()
    for s in range(F - 1):
        for d in (0, 1):

            @pl.when(jnp.logical_and(arrives(d, s), onward(d)))
            def _():
                for p in range(NP):
                    fs_copy(d, s, p).wait_send()
                if plan.dup:
                    dup_copy(d, s).wait_send()
    for j in range(1, R):
        rc(ysend.at[pl.ds(0, H)], yrecv.at[j], rys.at[j], ryr.at[j], "rep", rep_peer(j)).wait_send()
        half_copy(j).wait_send()
    for j in range(1, F):

        @pl.when(fs_peer(j) < O)
        def _():
            slice_copy(j).wait_send()

        @pl.when(z < O)
        def _():
            sum_copy(j).wait_send()
    for j in range(1, T):
        sq_copy(j).wait_send()


def exchange(plan, *args):
    F, R, T, NP, C = plan.F, plan.R, plan.T, plan.pieces, plan.cols
    f32 = jnp.float32
    vmem = pl.BlockSpec(memory_space=pltpu.VMEM)
    hbm = pl.BlockSpec(memory_space=pltpu.HBM)
    dma = pltpu.SemaphoreType.DMA
    rank = plan.rank
    out_shape = (
        jax.ShapeDtypeStruct((F, R, plan.rows, C), jnp.bfloat16),
        jax.ShapeDtypeStruct((rank, C), GATHER_TYPE),
        jax.ShapeDtypeStruct((8, 128), f32),
    ) + tuple(jax.ShapeDtypeStruct(a.shape, a.dtype) for a in args[3:])
    scratch = [pltpu.VMEM(a.shape, a.dtype) for a in args[:3]]
    scratch += [
        pltpu.VMEM((rank, C), f32),
        pltpu.VMEM((rank, C), REP_TYPE),
        pltpu.VMEM((R, plan.half, C), REP_TYPE),
        pltpu.VMEM((plan.half, C), f32),
        pltpu.VMEM((plan.half, C), FS_TYPE),
        pltpu.VMEM((F, plan.slice, C), FS_TYPE),
        pltpu.VMEM((T, 8, 128), f32),
        dma((11,)),
        dma((2, F, NP)),
        dma((2, F, NP)),
        dma((F, NP, R)),
        dma((F, NP, R)),
        dma((2, F)),
        dma((2, F)),
        dma((R,)), dma((R,)),
        dma((F,)), dma((F,)),
        dma((F,)), dma((F,)),
        dma((R,)), dma((R,)),
        dma((T,)), dma((T,)),
    ]
    return pl.pallas_call(
        functools.partial(kernel, plan),
        out_shape=out_shape,
        in_specs=[hbm] * 11,
        out_specs=[vmem] * 11,
        scratch_shapes=scratch,
        compiler_params=pltpu.CompilerParams(
            collective_id=0, has_side_effects=True, vmem_limit_bytes=40 * 1024 * 1024
        ),
    )(*(pltpu.with_memory_space_constraint(a, pltpu.HBM) for a in args))


BLOCKS = 8


def finish(
    plan, kfac, vfac, kw, vw, kf, ks, vf, vs, wall, total, squares,
    kw_out, vw_out, kf_out, ks_out, vf_out, vs_out, kstep_out, vstep_out, kcopy_out, vcopy_out,
    kw_new, vw_new, kf_new, ks_new, vf_new, vs_new, kstep, vstep, kcopy, vcopy, sem, copy_sem,
):
    me = lax.axis_index("fs") * plan.R + lax.axis_index("rep")
    mine = pl.ds(me * plan.rows, plan.rows)
    entries = jnp.float32(plan.rank * plan.cols * plan.T)
    shrink = jnp.sqrt(entries / (entries + squares[0:1, 0:1]))
    depth = kfac.shape[0] // BLOCKS

    def out(i, src, dst):
        c = pltpu.make_async_copy(src, dst, sem.at[i])
        c.start()
        return c

    sides = (
        (0, plan.kc, kfac, kw, kf, ks, (kf_new, ks_new, kstep, kw_new), (kf_out, ks_out, kstep_out, kw_out)),
        (plan.kc, plan.cols, vfac, vw, vf, vs, (vf_new, vs_new, vstep, vw_new), (vf_out, vs_out, vstep_out, vw_out)),
    )
    pending, uppers, lowers = [], [], []
    for k, (lo, hi, _, _, first, second, news, outs) in enumerate(sides):
        proj = total[:, lo:hi].astype(jnp.float32)
        first_new, second_new, normed = moments(proj, first[...], second[...])
        news[0][...] = first_new
        news[1][...] = second_new
        upper = normed.astype(jnp.bfloat16)
        uppers.append(upper)
        lowers.append((normed - upper.astype(jnp.float32)).astype(jnp.bfloat16))
        for i in (0, 1):
            pending.append(out(4 * k + i, news[i], outs[i]))

    for b in range(BLOCKS):
        rows = pl.ds(b * depth, depth)
        for k, (dst, dst_out) in enumerate(((kcopy, kcopy_out), (vcopy, vcopy_out))):
            lo, hi, factor = sides[k][:3]
            full = jnp.dot(factor[rows, :], uppers[k], preferred_element_type=jnp.float32)
            step = shrink * full
            dst[rows, :] = (wall[rows, lo:hi].astype(jnp.float32) - learn_rate * step).astype(
                jnp.bfloat16
            )
            c = pltpu.make_async_copy(dst.at[rows], dst_out.at[rows], copy_sem.at[k, b])
            c.start()
            pending.append(c)

    for k, (lo, hi, factor, weight, _, _, news, outs) in enumerate(sides):
        part = factor[mine, :]
        step = jnp.dot(part, uppers[k], preferred_element_type=jnp.float32)
        step = shrink * (step + jnp.dot(part, lowers[k], preferred_element_type=jnp.float32))
        news[2][...] = step
        news[3][...] = weight[...] - learn_rate * step
        for i in (2, 3):
            pending.append(out(4 * k + i, news[i], outs[i]))
    for c in pending:
        c.wait()


def body(mesh_shape, *args):
    (x, kcot, vcot, kfac, vfac, kw, vw, kf, ks, vf, vs) = args
    rows, key_cols = kw.shape
    value_cols = vw.shape[1]
    plan = Plan(mesh_shape, rows, kf.shape[0], key_cols, value_cols)
    wall, total, squares, *held = exchange(plan, *args)
    wall = wall.reshape(-1, plan.cols)
    like = [jax.ShapeDtypeStruct(a.shape, a.dtype) for a in (kw, vw, kf, ks, vf, vs, kw, vw)]
    depth = kfac.shape[0]
    like += [jax.ShapeDtypeStruct((depth, c), jnp.bfloat16) for c in (key_cols, value_cols)]
    vmem = pl.BlockSpec(memory_space=pltpu.VMEM)
    return pl.pallas_call(
        functools.partial(finish, plan),
        out_shape=like,
        in_specs=[vmem] * 11,
        out_specs=[pl.BlockSpec(memory_space=pl.ANY)] * 10,
        scratch_shapes=[pltpu.VMEM(a.shape, a.dtype) for a in like]
        + [pltpu.SemaphoreType.DMA((8,)), pltpu.SemaphoreType.DMA((2, BLOCKS))],
        compiler_params=pltpu.CompilerParams(vmem_limit_bytes=20 * 1024 * 1024),
    )(*held, wall, total, squares)


def solution(mesh):
    rows = P(("fs", "rep"), "tp")
    cols = P(None, "tp")
    in_specs = (P(("fs", "rep"), None), rows, rows, P(), P(), rows, rows, cols, cols, cols, cols)
    out_specs = (rows, rows, cols, cols, cols, cols, rows, rows, cols, cols)
    return jax.shard_map(
        functools.partial(body, dict(mesh.shape)),
        mesh=mesh, in_specs=in_specs, out_specs=out_specs, check_vma=False,
    )
```
